128 devices in a mesh: sp: 64 (over z, y, x), tp: 2 (over core).
Axes of the slice: x: 4, y: 4, z: 4, core: 2. Of those that a mesh axis runs over, the one named last changes fastest.
Arguments:
- conv_value: bfloat16 [16384, 1024], P('sp', 'tp'), may hold values from -6 to 6
- conv_gate: bfloat16 [16384, 1024], P('sp', 'tp'), may hold values from -6 to 6
- taps: bfloat16 [31, 1024], P(None, 'tp'), may hold values from -1 to 1
- doc_ids: int32 [16384], P('sp'), may hold values from 0 to 15, never falling along the last dimension, each value on 1 to 2048 neighbouring positions
- gn_gain: float32 [1024], P('tp'), may hold values from 0.1 to 1.9
- gn_shift: float32 [1024], P('tp'), may hold values from -3 to 3
- conv_out: bfloat16 [1024, 2048], replicated, may hold values from -0.1875 to 0.1875
- residual: bfloat16 [16384, 2048], P(('sp', 'tp')), may hold values from -6 to 6
- norm_gain: float32 [2048], replicated, may hold values from 0.1 to 1.9
- routes: int32 [16384, 2], P(('sp', 'tp')), may hold values from 0 to 127, as said below
- route_weight: float32 [16384, 2], P(('sp', 'tp')), may hold values from 0.3 to 1.2
- expert_gate: bfloat16 [128, 2048, 512], P(('sp', 'tp')), may hold values from -0.125 to 0.125
- expert_up: bfloat16 [128, 2048, 512], P(('sp', 'tp')), may hold values from -0.125 to 0.125
- expert_down: bfloat16 [128, 512, 2048], P(('sp', 'tp')), may hold values from -0.25 to 0.25
- shared_gate: bfloat16 [2048, 512], replicated, may hold values from -0.125 to 0.125
- shared_up: bfloat16 [2048, 512], replicated, may hold values from -0.125 to 0.125
- shared_down: bfloat16 [512, 2048], replicated, may hold values from -0.25 to 0.25
Outputs:
- layer_out: bfloat16 [16384, 2048], P(('sp', 'tp'))
The draws below stay inside these ranges and needn't reach their ends.
Inputs may be any that keep to these rules, and one draw needn't show every extreme that they name: `routes`: each row names 2 different experts. The rows of one device name each expert at most 4 times, and one expert, the same for every device, exactly 4 times. `doc_ids`: numbers never fall from one position to the next.
All inputs are finite; a program needn't handle non-finite values.
Results may differ from the reference program's by a relative error of at most 0.014.
Values may be sent and summed in bfloat16 or wider, within the bound.
No kernel may reach another device: no remote copies, remote signals or barrier semaphores. Data moves between devices by JAX's collectives and lax.ppermute only.
A program may use at most 128 MiB of HBM per device.

```python
import math
import jax
import jax.numpy as jnp
import numpy as np
from jax import lax

D = 2048
CONV_DIM = 1024
GROUPS = 8
WIDTH = 31
EXPERT_DIM = 512
SHARED_DIM = 512
TOP_K = 2
TOK_SP = 256
TOK_DEV = 128
TOKENS = 16384
EXPERTS = 128
CAP = 4
DOCS = 16


def draw_routes(key, part):
    blocks = TOKENS // TOK_DEV
    pairs = EXPERTS // 2
    key_order = jax.random.fold_in(key, 11)
    key_tilt = jax.random.fold_in(key, 12)
    key_noise = jax.random.fold_in(key, 13)
    key_rows = jax.random.fold_in(key, 14)
    order = jax.random.permutation(key_order, EXPERTS).astype(jnp.int32)
    tilt = jax.random.randint(key_tilt, (pairs,), 0, CAP + 1)
    noise = jax.random.randint(key_noise, (blocks, pairs), -(CAP // 4), CAP // 4 + 1)
    first = jnp.clip(tilt[None, :] + noise, 0, CAP)
    first = first.at[:, 0].set(CAP)
    pair_counts = jnp.stack([first, CAP - first], axis=2).reshape(blocks, EXPERTS)
    counts = jnp.zeros((blocks, EXPERTS), jnp.int32).at[:, order].set(pair_counts.astype(jnp.int32))
    cumulative = jnp.cumsum(counts, axis=1).astype(jnp.int32)
    positions = jnp.arange(TOK_DEV * TOP_K, dtype=jnp.int32)
    expert_of = jax.vmap(lambda row: jnp.searchsorted(row, positions, side='right'))(cumulative).astype(jnp.int32)
    slots = expert_of.reshape(blocks, TOP_K, TOK_DEV).transpose(0, 2, 1)
    row_keys = jax.random.split(key_rows, blocks)
    shuffles = jax.vmap(lambda one_key: jax.random.permutation(one_key, TOK_DEV))(row_keys).astype(jnp.int32)
    shuffles = jnp.broadcast_to(shuffles[:, :, None], (blocks, TOK_DEV, TOP_K))
    shuffled = jnp.take_along_axis(slots, shuffles, axis=1)
    return shuffled.reshape(TOKENS, TOP_K).astype(jnp.int32)


def level_of(key, extent, shards, low, high):
    loudness = 1.0
    for dim, parts in shards:
        draws = jax.random.uniform(jax.random.fold_in(jax.random.fold_in(key, 6), dim), (parts,), jnp.float32, low / len(shards), high / len(shards))
        loudness = loudness * jnp.repeat(jnp.exp(draws), extent[dim] // parts).reshape((-1,) + (1,) * (len(extent) - 1 - dim))
    return loudness


def length_profile(count, total, reach, slope):
    weights = [(1 << 20) // math.isqrt(rank ** slope) + 1 for rank in range(2, count + 1)]
    rest, holding = total - reach - (count - 1), [1] * (count - 1)
    while rest > 0:
        candidates = [i for i in range(count - 1) if holding[i] < reach]
        pool, left = sum([weights[i] for i in candidates]), rest
        for i in candidates:
            more = min(reach - holding[i], max(1, left * weights[i] // pool), rest)
            holding[i] = holding[i] + more
            rest = rest - more
    return np.array([reach] + holding)


def uneven_parts(own_key, amount, total, bound, lean):
    if amount == 2:
        one = jax.random.randint(own_key, (), max(1, total - bound), min(bound, total - 1) + 1)
        return jnp.stack([one, total - one])
    sizes = jnp.asarray(length_profile(amount, total, bound, lean), jnp.int32)
    couples = (amount - 1) // 2
    giver, taker = sizes[1:1 + 2 * couples:2], sizes[2:2 + 2 * couples:2]
    room = jnp.minimum(giver - 1, bound - taker)
    moved = jax.random.randint(jax.random.fold_in(own_key, 1), (couples,), 0, 1 << 20) % (room + 1)
    sizes = sizes.at[1:1 + 2 * couples:2].set(giver - moved).at[2:2 + 2 * couples:2].set(taker + moved)
    return sizes[jax.random.permutation(jax.random.fold_in(own_key, 2), amount)]


def normal_values(own_key, dims, scale, most, cuts=(), kind=jnp.bfloat16):
    array = scale * jax.random.normal(own_key, dims, jnp.float32)
    if cuts:
        array = array * level_of(own_key, dims, cuts, -0.22, 0.18)
    return jnp.clip(array, -most, most).astype(kind)


def setup_inputs(seed: int = 0) -> dict:
    arg_keys = jax.random.split(jax.random.key(seed), 18)
    return {
        "conv_value": normal_values(arg_keys[0], (TOKENS, CONV_DIM), 1.0, 6.0, ((0, 64), (1, 2))),
        "conv_gate": normal_values(arg_keys[1], (TOKENS, CONV_DIM), 1.0, 6.0, ((0, 64), (1, 2))),
        "taps": normal_values(arg_keys[2], (WIDTH, CONV_DIM), WIDTH ** -0.5, 1.0, ((1, 2),)),
        "doc_ids": jnp.searchsorted(jnp.cumsum(uneven_parts(arg_keys[3], DOCS, TOKENS, 8 * TOK_SP, 1)), jnp.arange(TOKENS), side="right").astype(jnp.int32),
        "gn_gain": jnp.clip(1.0 + 0.18 * jax.random.normal(arg_keys[4], (CONV_DIM,), jnp.float32), 0.1, 1.9),
        "gn_shift": normal_values(arg_keys[5], (CONV_DIM,), 0.5, 3.0, ((0, 2),), jnp.float32),
        "conv_out": normal_values(arg_keys[6], (CONV_DIM, D), CONV_DIM ** -0.5, 0.1875),
        "residual": normal_values(arg_keys[7], (TOKENS, D), 1.0, 6.0, ((0, 128),)),
        "norm_gain": jnp.clip(1.0 + 0.18 * jax.random.normal(arg_keys[8], (D,), jnp.float32), 0.1, 1.9),
        "routes": draw_routes(jax.random.fold_in(arg_keys[17], 71), 0),
        "route_weight": jnp.clip(0.3 + 0.90000004 * jax.random.uniform(arg_keys[10], (TOKENS, TOP_K), jnp.float32) ** level_of(arg_keys[10], (TOKENS, TOP_K), ((0, 128),), -0.2, 0.2), 0.3, 1.2),
        "expert_gate": normal_values(arg_keys[11], (EXPERTS, D, EXPERT_DIM), D ** -0.5, 0.125, ((0, 128),)),
        "expert_up": normal_values(arg_keys[12], (EXPERTS, D, EXPERT_DIM), D ** -0.5, 0.125, ((0, 128),)),
        "expert_down": normal_values(arg_keys[13], (EXPERTS, EXPERT_DIM, D), EXPERT_DIM ** -0.5, 0.25, ((0, 128),)),
        "shared_gate": normal_values(arg_keys[14], (D, SHARED_DIM), D ** -0.5, 0.125),
        "shared_up": normal_values(arg_keys[15], (D, SHARED_DIM), D ** -0.5, 0.125),
        "shared_down": normal_values(arg_keys[16], (SHARED_DIM, D), SHARED_DIM ** -0.5, 0.25),
    }


epsilon = 1e-06

def route_rows(normed, routes, route_weight, expert_gate, expert_up, expert_down):
    blocks = TOKENS // TOK_DEV
    flat_routes = routes.reshape(blocks, TOK_DEV * TOP_K).astype(jnp.int32)
    onehot = (flat_routes[:, :, None] == jnp.arange(EXPERTS, dtype=jnp.int32)[None, None, :]).astype(jnp.int32)
    slot_index = (lax.optimization_barrier(jnp.sum(jnp.cumsum(onehot, axis=1) * onehot, axis=2)) - 1).astype(jnp.int32)
    block_index = jnp.broadcast_to(jnp.arange(blocks, dtype=jnp.int32)[:, None], flat_routes.shape)
    row_index = (block_index * TOK_DEV + jnp.arange(TOK_DEV * TOP_K, dtype=jnp.int32)[None, :] // TOP_K).astype(jnp.int32)
    slot_table = jnp.full((EXPERTS, blocks, CAP), TOKENS, jnp.int32).at[flat_routes, block_index, slot_index].set(row_index)
    weight_table = jnp.zeros((EXPERTS, blocks, CAP), jnp.float32).at[flat_routes, block_index, slot_index].set(route_weight.reshape(blocks, TOK_DEV * TOP_K).astype(jnp.float32))
    padded_rows = jnp.concatenate([normed, jnp.zeros((1, D), normed.dtype)], axis=0)

    def one_expert(routed_sum, pieces):
        table_rows, table_weights, gate_weight, up_weight, down_weight = pieces
        expert_rows = padded_rows[table_rows]
        gate_part = jnp.dot(expert_rows, gate_weight, preferred_element_type=jnp.float32)
        up_part = jnp.dot(expert_rows, up_weight, preferred_element_type=jnp.float32)
        hidden = (jax.nn.silu(gate_part) * up_part).astype(jnp.bfloat16)
        result = jnp.dot(hidden, down_weight, preferred_element_type=jnp.float32).astype(jnp.bfloat16)
        routed_sum = routed_sum.at[table_rows].add(table_weights[:, None] * result.astype(jnp.float32), mode='drop')
        return (routed_sum, None)
    routed, _ = lax.scan(one_expert, jnp.zeros((TOKENS, D), jnp.float32), (slot_table.reshape(EXPERTS, blocks * CAP), weight_table.reshape(EXPERTS, blocks * CAP), expert_gate, expert_up, expert_down))
    return routed

def reference(conv_value, conv_gate, taps, doc_ids, gn_gain, gn_shift, conv_out, residual, norm_gain, routes, route_weight, expert_gate, expert_up, expert_down, shared_gate, shared_up, shared_down):
    glu = (conv_value.astype(jnp.float32) * jax.nn.sigmoid(conv_gate.astype(jnp.float32))).astype(jnp.bfloat16)
    padded_glu = jnp.pad(glu, ((WIDTH - 1, 0), (0, 0)))
    padded_ids = jnp.pad(doc_ids, (WIDTH - 1, 0), constant_values=-1)
    conv_sum = jnp.zeros((TOKENS, CONV_DIM), jnp.float32)
    for offset in range(WIDTH):
        same_doc = (padded_ids[offset:offset + TOKENS] == doc_ids)[:, None]
        tap_term = taps[offset].astype(jnp.float32)[None, :] * padded_glu[offset:offset + TOKENS].astype(jnp.float32)
        conv_sum = conv_sum + jnp.where(same_doc, tap_term, 0.0)
    grouped = conv_sum.reshape(TOKENS, GROUPS, CONV_DIM // GROUPS)
    group_mean = lax.optimization_barrier(jnp.mean(grouped, axis=-1, keepdims=True))
    centered = grouped - group_mean
    group_var = lax.optimization_barrier(jnp.mean(centered * centered, axis=-1, keepdims=True))
    normalized = (centered * lax.rsqrt(group_var + epsilon)).reshape(TOKENS, CONV_DIM)
    conv_act = jax.nn.silu(normalized * gn_gain + gn_shift).astype(jnp.bfloat16)
    projected = jnp.dot(conv_act, conv_out, preferred_element_type=jnp.float32)
    stream = (residual.astype(jnp.float32) + projected).astype(jnp.bfloat16)
    stream_wide = stream.astype(jnp.float32)
    normed = (stream_wide * lax.rsqrt(lax.optimization_barrier(jnp.mean(stream_wide * stream_wide, axis=-1, keepdims=True)) + epsilon) * norm_gain).astype(jnp.bfloat16)
    shared_hidden = (jax.nn.silu(jnp.dot(normed, shared_gate, preferred_element_type=jnp.float32)) * jnp.dot(normed, shared_up, preferred_element_type=jnp.float32)).astype(jnp.bfloat16)
    shared_out = jnp.dot(shared_hidden, shared_down, preferred_element_type=jnp.float32)
    routed = route_rows(normed, routes, route_weight, expert_gate, expert_up, expert_down)
    return (stream_wide + shared_out + routed).astype(jnp.bfloat16)
```

```python
import functools

import jax
import jax.numpy as jnp
from jax import lax
from jax.experimental import pallas as pl
from jax.experimental.pallas import tpu as pltpu
from jax.sharding import PartitionSpec as P

GROUPS = 8
EPS = 1e-06
F32 = jnp.float32
BF16 = jnp.bfloat16
HALO = 32
PACK = 40


def from_behind(x, axis, by):
    peers = lax.axis_size(axis)
    pairs = [(i, i + by) for i in range(peers) if 0 <= i + by < peers]
    return lax.ppermute(x, axis, pairs)


def glu_of(value, gate):
    wide = value.astype(F32) * jax.nn.sigmoid(gate.astype(F32))
    return wide.astype(BF16)


def pack_kernel(value, gate, ids, out):
    channels = value.shape[1]
    positions = ids.shape[1]
    out[0:HALO, :] = glu_of(value[...], gate[...])
    tail = ids[:, positions - 128 :].astype(F32)
    row = jnp.concatenate([tail, jnp.zeros((1, channels - 128), F32)], axis=1)
    out[HALO:, :] = jnp.broadcast_to(row, (PACK - HALO, channels)).astype(BF16)


def conv_kernel(value, gate, taps, ids, halo_ids, halo, gain, shift, out, ext, moved, depth):
    positions = value.shape[0]
    width = taps.shape[0]

    @pl.when(pl.program_id(0) == 0)
    def _():
        own = ids[...].astype(F32)
        own8 = jnp.broadcast_to(own, (8, positions))
        column = jnp.transpose(own8)[:, 0:1]
        t = lax.broadcasted_iota(jnp.int32, (positions, positions), 0)
        s = lax.broadcasted_iota(jnp.int32, (positions, positions), 1)
        near = (column == own) & (s < t) & (s > t - width)
        t = lax.broadcasted_iota(jnp.int32, (positions, 128), 0)
        s = lax.broadcasted_iota(jnp.int32, (positions, 128), 1)
        behind = (column == halo_ids[0:1, :].astype(F32)) & (s - 128 > t - width)
        count = jnp.dot(
            near.astype(F32).astype(BF16), jnp.ones((positions, 128), BF16), preferred_element_type=F32
        )
        count = count + jnp.dot(
            behind.astype(F32).astype(BF16), jnp.ones((128, 128), BF16), preferred_element_type=F32
        )
        depth[...] = count

    ext[0:HALO, :] = halo[0:HALO, :].astype(F32)
    ext[HALO : HALO + positions, :] = glu_of(value[...], gate[...]).astype(F32)
    ext[HALO + positions :, :] = jnp.zeros((8, 128), F32)
    span = HALO + positions
    for r in range(1, 8):
        moved[r, :, :] = ext[pl.ds(r, span), :]
    rows = 64
    for base in range(0, positions, rows):
        deep = depth[base : base + rows, :]
        total = jnp.zeros((rows, 128), F32)
        for i in range(width):
            start = HALO - (width - 1) + i
            r = start % 8
            at = base + start - r
            x = ext[at : at + rows, :] if r == 0 else moved[r, at : at + rows, :]
            term = taps[i : i + 1, :].astype(F32) * x
            lag = width - 1 - i
            total = total + (jnp.where(deep >= lag, term, 0.0) if lag else term)
        mean = jnp.mean(total, axis=-1, keepdims=True)
        centered = total - mean
        var = jnp.mean(centered * centered, axis=-1, keepdims=True)
        v = centered * lax.rsqrt(var + EPS) * gain[...] + shift[...]
        out[base : base + rows, :] = jax.nn.silu(v).astype(BF16)


def spread_kernel(act, conv_out, residual, norm_gain, routes, weights, stream, normed, outgoing, meta, wide):
    step = pl.program_id(0)
    tokens = act.shape[1]
    half_in = act.shape[2]
    columns = conv_out.shape[1]
    steps = wide.shape[0]
    part = jnp.dot(act[0], conv_out[0:half_in, :], preferred_element_type=F32)
    part = part + jnp.dot(act[1], conv_out[half_in:, :], preferred_element_type=F32)
    wide[step] = (residual[...].astype(F32) + part).astype(BF16).astype(F32)

    @pl.when(step == steps - 1)
    def _():
        blocks = [wide[n] for n in range(steps)]
        square = sum(jnp.sum(b * b, axis=-1, keepdims=True) for b in blocks)
        model_width = columns * steps
        scale = lax.rsqrt(square / model_width + EPS)
        for n, b in enumerate(blocks):
            at = n * columns
            stream[:, at : at + columns] = b.astype(BF16)
            normed[:, at : at + columns] = (b * scale * norm_gain[:, at : at + columns]).astype(BF16)
        experts = outgoing.shape[0] // 8
        expert = lax.broadcasted_iota(jnp.int32, (experts, tokens), 0)
        hot = [(expert == routes[k : k + 1, :]).astype(F32) for k in range(2)]
        a = lax.broadcasted_iota(jnp.int32, (tokens, tokens), 0)
        b = lax.broadcasted_iota(jnp.int32, (tokens, tokens), 1)
        before = (a < b).astype(F32).astype(BF16)
        ahead = [jnp.dot(h.astype(BF16), before, preferred_element_type=F32) for h in hot]
        ahead[1] = ahead[1] + jnp.sum(hot[0], axis=1, keepdims=True)
        slot = [jnp.sum(h * c, axis=0, keepdims=True) for h, c in zip(hot, ahead)]
        target = [routes[k : k + 1, :].astype(F32) * 4.0 + slot[k] for k in range(2)]
        meta[...] = jnp.concatenate(
            target + [weights[0:1, :], weights[1:2, :], jnp.zeros((4, tokens), F32)], axis=0
        )
        r = lax.broadcasted_iota(jnp.int32, (8 * experts, tokens), 0)
        slots = ((r // 8) * 4 + r % 4).astype(F32)
        half = (r // 4) % 2
        chosen = (slots == target[0]) | (slots == target[1])
        pick = jnp.concatenate(
            [(chosen & (half == h)).astype(F32).astype(BF16) for h in range(2)], axis=1
        )
        mid = model_width // 2
        source = jnp.concatenate([normed[:, 0:mid], normed[:, mid:]], axis=0)
        outgoing[...] = jnp.dot(pick, source, preferred_element_type=F32).astype(BF16)


def expert_kernel(x, gate, up, down, out):
    rows, half = x.shape
    quads = rows // 16
    wide = x[...].astype(F32).reshape(quads, 2, 8, half)
    a, b = wide[:, 0], wide[:, 1]
    low = lax.broadcasted_iota(jnp.int32, (quads, 8, half), 1) < 4
    top = jnp.where(low, a, pltpu.roll(b, 4, 1)).reshape(quads * 8, half).astype(BF16)
    bottom = jnp.where(low, pltpu.roll(a, 4, 1), b).reshape(quads * 8, half).astype(BF16)

    def apply(w):
        return jnp.dot(top, w[0:half, :], preferred_element_type=F32) + jnp.dot(
            bottom, w[half:, :], preferred_element_type=F32
        )

    hidden = (jax.nn.silu(apply(gate)) * apply(up)).astype(BF16)
    left = jnp.dot(hidden, down[:, 0:half], preferred_element_type=F32).reshape(quads, 8, half)
    right = jnp.dot(hidden, down[:, half:], preferred_element_type=F32).reshape(quads, 8, half)
    first = jnp.where(low, left, pltpu.roll(right, 4, 1))
    second = jnp.where(low, pltpu.roll(left, 4, 1), right)
    out[...] = jnp.stack([first, second], axis=1).reshape(rows, half).astype(BF16)


def shared_kernel(normed, gate, up, down, out):
    rows = normed[...]
    g = jnp.dot(rows, gate[...], preferred_element_type=F32)
    u = jnp.dot(rows, up[...], preferred_element_type=F32)
    hidden = (jax.nn.silu(g) * u).astype(BF16)
    part = jnp.dot(hidden, down[...], preferred_element_type=F32)

    @pl.when(pl.program_id(0) == 0)
    def _():
        out[...] = part

    @pl.when(pl.program_id(0) > 0)
    def _():
        out[...] += part


def gather_kernel(returned, meta, stream, shared, out):
    rows, half = returned.shape
    tokens = stream.shape[0]
    columns = jnp.transpose(meta[...])
    r = lax.broadcasted_iota(jnp.int32, (tokens, rows), 1)
    slots = ((r // 8) * 4 + r % 4).astype(F32)
    side = (r // 4) % 2
    weight = jnp.where(
        slots == columns[:, 0:1],
        columns[:, 2:3],
        jnp.where(slots == columns[:, 1:2], columns[:, 3:4], 0.0),
    )
    high = weight.astype(BF16)
    low = (weight - high.astype(F32)).astype(BF16)
    zero = jnp.zeros_like(weight)
    for h in range(2):
        at = h * half
        here = side == h
        first = jnp.where(here, high.astype(F32), zero).astype(BF16)
        second = jnp.where(here, low.astype(F32), zero).astype(BF16)
        routed = jnp.dot(first, returned[...], preferred_element_type=F32) + jnp.dot(
            second, returned[...], preferred_element_type=F32
        )
        base = stream[:, at : at + half].astype(F32) + shared[:, at : at + half]
        out[:, at : at + half] = (base + routed).astype(BF16)


def full(shape):
    zeros = (0,) * len(shape)
    return pl.BlockSpec(shape, lambda *_: zeros)


def per_device(
    conv_value,
    conv_gate,
    taps,
    doc_ids,
    gn_gain,
    gn_shift,
    conv_out,
    residual,
    norm_gain,
    routes,
    route_weight,
    expert_gate,
    expert_up,
    expert_down,
    shared_gate,
    shared_up,
    shared_down,
):
    positions, channels = conv_value.shape
    width = taps.shape[0]
    tokens, model_width = residual.shape
    experts = expert_gate.shape[0] * lax.axis_size("sp") * lax.axis_size("tp")
    half = model_width // 2
    ids = doc_ids.reshape(1, positions)
    sds = jax.ShapeDtypeStruct

    last = positions // HALO - 1
    packed = pl.pallas_call(
        pack_kernel,
        grid=(1,),
        in_specs=[
            pl.BlockSpec((HALO, channels), lambda i: (last, 0)),
            pl.BlockSpec((HALO, channels), lambda i: (last, 0)),
            full((1, positions)),
        ],
        out_specs=full((PACK, channels)),
        out_shape=sds((PACK, channels), BF16),
        name="pack",
    )(conv_value, conv_gate, ids)
    halo = from_behind(packed, "sp", 1)

    act = pl.pallas_call(
        conv_kernel,
        grid=(channels // 128,),
        in_specs=[
            pl.BlockSpec((positions, 128), lambda i: (0, i)),
            pl.BlockSpec((positions, 128), lambda i: (0, i)),
            pl.BlockSpec((width, 128), lambda i: (0, i)),
            full((1, positions)),
            pl.BlockSpec((8, 128), lambda i: (HALO // 8, 0)),
            pl.BlockSpec((HALO, 128), lambda i: (0, i)),
            pl.BlockSpec((1, 128), lambda i: (0, i)),
            pl.BlockSpec((1, 128), lambda i: (0, i)),
        ],
        out_specs=pl.BlockSpec((positions, 128), lambda i: (0, i)),
        out_shape=sds((positions, channels), BF16),
        scratch_shapes=[
            pltpu.VMEM((HALO + positions + 8, 128), F32),
            pltpu.VMEM((8, HALO + positions, 128), F32),
            pltpu.VMEM((positions, 128), F32),
        ],
        name="conv",
    )(
        conv_value,
        conv_gate,
        taps,
        ids,
        halo,
        halo,
        gn_gain.reshape(1, channels),
        gn_shift.reshape(1, channels),
    )
    both = lax.all_to_all(
        act.reshape(2, tokens, channels), "tp", split_axis=0, concat_axis=0, tiled=True
    )

    steps = 4
    block = model_width // steps
    stream, normed, outgoing, meta = pl.pallas_call(
        spread_kernel,
        grid=(steps,),
        in_specs=[
            full((2, tokens, channels)),
            pl.BlockSpec((2 * channels, block), lambda i: (0, i)),
            pl.BlockSpec((tokens, block), lambda i: (0, i)),
            full((1, model_width)),
            full((2, tokens)),
            full((2, tokens)),
        ],
        out_specs=[
            full((tokens, model_width)),
            full((tokens, model_width)),
            full((8 * experts, half)),
            full((8, tokens)),
        ],
        out_shape=[
            sds((tokens, model_width), BF16),
            sds((tokens, model_width), BF16),
            sds((8 * experts, half), BF16),
            sds((8, tokens), F32),
        ],
        scratch_shapes=[pltpu.VMEM((steps, tokens, block), F32)],
        name="spread",
    )(both, conv_out, residual, norm_gain.reshape(1, model_width), routes.T, route_weight.T)

    exchange = functools.partial(
        lax.all_to_all, axis_name=("sp", "tp"), split_axis=0, concat_axis=0, tiled=True
    )
    arrived = exchange(outgoing.reshape(experts, 8, half)).reshape(8 * experts, half)

    hidden = shared_gate.shape[1]
    piece = 128
    shared = pl.pallas_call(
        shared_kernel,
        grid=(hidden // piece,),
        in_specs=[
            full((tokens, model_width)),
            pl.BlockSpec((model_width, piece), lambda i: (0, i)),
            pl.BlockSpec((model_width, piece), lambda i: (0, i)),
            pl.BlockSpec((piece, model_width), lambda i: (i, 0)),
        ],
        out_specs=full((tokens, model_width)),
        out_shape=sds((tokens, model_width), F32),
        cost_estimate=pl.CostEstimate(flops=8_000_000_000, bytes_accessed=8_000_000, transcendentals=0),
        name="shared",
    )(normed, shared_gate, shared_up, shared_down)

    hidden = expert_gate.shape[2]
    chunk = 2 * experts
    result = pl.pallas_call(
        expert_kernel,
        grid=(8 * experts // chunk,),
        in_specs=[
            pl.BlockSpec((chunk, half), lambda i: (i, 0)),
            full((model_width, hidden)),
            full((model_width, hidden)),
            full((hidden, model_width)),
        ],
        out_specs=pl.BlockSpec((chunk, half), lambda i: (i, 0)),
        out_shape=sds((8 * experts, half), BF16),
        name="expert",
    )(arrived, expert_gate[0], expert_up[0], expert_down[0])
    returned = exchange(result.reshape(experts, 8, half)).reshape(8 * experts, half)

    return pl.pallas_call(
        gather_kernel,
        out_shape=sds((tokens, model_width), BF16),
        name="gather",
    )(returned, meta, stream, shared)


def solution(mesh):
    return jax.shard_map(
        per_device,
        mesh=mesh,
        in_specs=(
            P("sp", "tp"),
            P("sp", "tp"),
            P(None, "tp"),
            P("sp"),
            P("tp"),
            P("tp"),
            P(),
            P(("sp", "tp"), None),
            P(),
            P(("sp", "tp"), None),
            P(("sp", "tp"), None),
            P(("sp", "tp"), None, None),
            P(("sp", "tp"), None, None),
            P(("sp", "tp"), None, None),
            P(),
            P(),
            P(),
        ),
        out_specs=P(("sp", "tp"), None),
        check_vma=False,
    )
```

```python
import functools

import jax
import jax.numpy as jnp
from jax import lax
from jax.experimental import pallas as pl
from jax.experimental.pallas import tpu as pltpu
from jax.sharding import PartitionSpec as P

GROUPS = 8
EPS = 1e-06
F32 = jnp.float32
BF16 = jnp.bfloat16
HALO = 32
PACK = 40


def from_behind(x, axis, by):
    peers = lax.axis_size(axis)
    pairs = [(i, (i + by) % peers) for i in range(peers)]
    return lax.ppermute(x, axis, pairs)


def glu_of(value, gate):
    wide = value.astype(F32) * jax.nn.sigmoid(gate.astype(F32))
    return wide.astype(BF16)


def pack_kernel(value, gate, ids, out):
    channels = value.shape[1]
    positions = ids.shape[1]
    out[0:HALO, :] = glu_of(value[...], gate[...])
    tail = ids[:, positions - 128 :].astype(F32)
    row = jnp.concatenate([tail, jnp.zeros((1, channels - 128), F32)], axis=1)
    out[HALO:, :] = jnp.broadcast_to(row, (PACK - HALO, channels)).astype(BF16)


def same_document(column, row, first, behind, width):
    shape = (column.shape[0], row.shape[1])
    t = lax.broadcasted_iota(jnp.int32, shape, 0) + first
    s = lax.broadcasted_iota(jnp.int32, shape, 1) - behind
    near = (column == row) & (s < t) & (s > t - width)
    ones = jnp.ones((shape[1], 128), BF16)
    return jnp.dot(near.astype(F32).astype(BF16), ones, preferred_element_type=F32)


def column_of(row):
    return jnp.transpose(jnp.broadcast_to(row, (8, row.shape[1])))[:, 0:1]


def normalized(fetch, deep, taps, gain, shift, lanes):
    width = taps.shape[0]
    total = jnp.zeros(deep.shape, F32)
    for i in range(width):
        term = taps[i : i + 1, lanes].astype(F32) * fetch(i)
        lag = width - 1 - i
        total = total + (jnp.where(deep >= lag, term, 0.0) if lag else term)
    mean = jnp.mean(total, axis=-1, keepdims=True)
    centered = total - mean
    var = jnp.mean(centered * centered, axis=-1, keepdims=True)
    v = centered * lax.rsqrt(var + EPS) * gain[:, lanes] + shift[:, lanes]
    return jax.nn.silu(v).astype(BF16)


def conv_kernel(value, gate, taps, ids, gain, shift, act, ext, moved, depth):
    positions, channels = value.shape
    width = taps.shape[0]
    own = ids[...].astype(F32)
    depth[...] = same_document(column_of(own), own, 0, 0, width)
    ext[positions:, :] = jnp.zeros((8, 128), F32)
    for c in range(channels // 128):
        lanes = slice(c * 128, c * 128 + 128)
        ext[0:positions, :] = glu_of(value[:, lanes], gate[:, lanes]).astype(F32)
        for r in range(1, 8):
            moved[r, :, :] = ext[pl.ds(r, positions), :]
        base = HALO
        while base < positions:
            rows = HALO if base == HALO else 2 * HALO

            def fetch(i, base=base, rows=rows):
                start = base - (width - 1) + i
                r = start % 8
                at = slice(start - r, start - r + rows)
                return ext[at, :] if r == 0 else moved[r, at, :]

            deep = depth[base : base + rows, :]
            act[base : base + rows, lanes] = normalized(fetch, deep, taps, gain, shift, lanes)
            base += rows


def rim_kernel(act, value, gate, taps, ids, halo, gain, shift, keep, send, ext, moved):
    channels = value.shape[1]
    rows = HALO
    width = taps.shape[0]
    tokens = keep.shape[0]
    mine = lax.axis_index("tp")
    own = ids[...].astype(F32)
    column = column_of(own)[0:rows]
    deep = same_document(column, own, 0, 0, width) + same_document(
        column, halo[HALO : HALO + 1, 0:128].astype(F32), 0, 128, width
    )
    at = pl.multiple_of(mine * tokens, tokens)
    keep[...] = act[pl.ds(at, tokens), :]
    at = pl.multiple_of((1 - mine) * tokens, tokens)
    send[...] = act[pl.ds(at, tokens), :]
    ext[2 * HALO :, :] = jnp.zeros((8, 128), F32)
    for c in range(channels // 128):
        lanes = slice(c * 128, c * 128 + 128)
        ext[0:HALO, :] = halo[0:HALO, lanes].astype(F32)
        ext[HALO : 2 * HALO, :] = glu_of(value[0:rows, lanes], gate[0:rows, lanes]).astype(F32)
        for r in range(1, 8):
            moved[r, :, :] = ext[pl.ds(r, 2 * HALO), :]

        def fetch(i):
            start = HALO - (width - 1) + i
            r = start % 8
            at = slice(start - r, start - r + rows)
            return ext[at, :] if r == 0 else moved[r, at, :]

        first = normalized(fetch, deep, taps, gain, shift, lanes)

        @pl.when(mine == 0)
        def _():
            keep[0:rows, lanes] = first

        @pl.when(mine == 1)
        def _():
            send[0:rows, lanes] = first


def route_kernel(routes, weights, meta, pick):
    tokens = routes.shape[1]
    experts = pick.shape[0] // 8
    expert = lax.broadcasted_iota(jnp.int32, (experts, tokens), 0)
    hot = [(expert == routes[k : k + 1, :]).astype(F32) for k in range(2)]
    a = lax.broadcasted_iota(jnp.int32, (tokens, tokens), 0)
    b = lax.broadcasted_iota(jnp.int32, (tokens, tokens), 1)
    before = (a < b).astype(F32).astype(BF16)
    ahead = [jnp.dot(h.astype(BF16), before, preferred_element_type=F32) for h in hot]
    ahead[1] = ahead[1] + jnp.sum(hot[0], axis=1, keepdims=True)
    slot = [jnp.sum(h * c, axis=0, keepdims=True) for h, c in zip(hot, ahead)]
    target = [routes[k : k + 1, :].astype(F32) * 4.0 + slot[k] for k in range(2)]
    meta[...] = jnp.concatenate(
        target + [weights[0:1, :], weights[1:2, :], jnp.zeros((4, tokens), F32)], axis=0
    )
    r = lax.broadcasted_iota(jnp.int32, (8 * experts, tokens), 0)
    slots = ((r // 8) * 4 + r % 4).astype(F32)
    half = (r // 4) % 2
    chosen = (slots == target[0]) | (slots == target[1])
    for h in range(2):
        pick[:, h * tokens : (h + 1) * tokens] = (chosen & (half == h)).astype(F32).astype(BF16)


def spread_kernel(keep, got, conv_out, residual, norm_gain, pick, stream, normed, outgoing):
    tokens, half_in = keep.shape
    model_width = residual.shape[1]
    mine = lax.axis_index("tp")
    first = pl.multiple_of(mine * half_in, half_in)
    other = pl.multiple_of((1 - mine) * half_in, half_in)
    part = jnp.dot(keep[...], conv_out[pl.ds(first, half_in), :], preferred_element_type=F32)
    part = part + jnp.dot(got[...], conv_out[pl.ds(other, half_in), :], preferred_element_type=F32)
    rows = (residual[...].astype(F32) + part).astype(BF16)
    stream[...] = rows
    wide = rows.astype(F32)
    scale = lax.rsqrt(jnp.mean(wide * wide, axis=-1, keepdims=True) + EPS)
    ready = (wide * scale * norm_gain[...]).astype(BF16)
    normed[...] = ready
    mid = model_width // 2
    source = jnp.concatenate([ready[:, 0:mid], ready[:, mid:]], axis=0)
    outgoing[...] = jnp.dot(pick[...], source, preferred_element_type=F32).astype(BF16)


def expert_kernel(x, gate, up, down, out):
    rows, half = out.shape
    at = pl.ds(pl.multiple_of(pl.program_id(0) * rows, rows), rows)
    quads = rows // 16
    wide = x[at, :].astype(F32).reshape(quads, 2, 8, half)
    a, b = wide[:, 0], wide[:, 1]
    low = lax.broadcasted_iota(jnp.int32, (quads, 8, half), 1) < 4
    top = jnp.where(low, a, pltpu.roll(b, 4, 1)).reshape(quads * 8, half).astype(BF16)
    bottom = jnp.where(low, pltpu.roll(a, 4, 1), b).reshape(quads * 8, half).astype(BF16)

    def apply(w):
        return jnp.dot(top, w[0:half, :], preferred_element_type=F32) + jnp.dot(
            bottom, w[half:, :], preferred_element_type=F32
        )

    hidden = (jax.nn.silu(apply(gate)) * apply(up)).astype(BF16)
    left = jnp.dot(hidden, down[:, 0:half], preferred_element_type=F32).reshape(quads, 8, half)
    right = jnp.dot(hidden, down[:, half:], preferred_element_type=F32).reshape(quads, 8, half)
    first = jnp.where(low, left, pltpu.roll(right, 4, 1))
    second = jnp.where(low, pltpu.roll(left, 4, 1), right)
    out[...] = jnp.stack([first, second], axis=1).reshape(rows, half).astype(BF16)


def shared_kernel(normed, stream, gate, up, down, out):
    rows = normed[...]
    g = jnp.dot(rows, gate[...], preferred_element_type=F32)
    u = jnp.dot(rows, up[...], preferred_element_type=F32)
    hidden = (jax.nn.silu(g) * u).astype(BF16)
    part = jnp.dot(hidden, down[...], preferred_element_type=F32)

    @pl.when(pl.program_id(0) == 0)
    def _():
        out[...] = stream[...].astype(F32) + part

    @pl.when(pl.program_id(0) > 0)
    def _():
        out[...] += part


def gather_kernel(returned, meta, base, out):
    rows, half = returned.shape
    tokens = base.shape[0]
    h = pl.program_id(0)
    columns = jnp.transpose(meta[...])
    r = lax.broadcasted_iota(jnp.int32, (tokens, rows), 1)
    slots = ((r // 8) * 4 + r % 4).astype(F32)
    here = (r // 4) % 2 == h
    weight = jnp.where(
        here & (slots == columns[:, 0:1]),
        columns[:, 2:3],
        jnp.where(here & (slots == columns[:, 1:2]), columns[:, 3:4], 0.0),
    )
    high = weight.astype(BF16)
    low = (weight - high.astype(F32)).astype(BF16)
    routed = jnp.dot(high, returned[...], preferred_element_type=F32) + jnp.dot(
        low, returned[...], preferred_element_type=F32
    )
    out[...] = (base[:, pl.ds(pl.multiple_of(h * half, half), half)] + routed).astype(BF16)


def whole(shape):
    zeros = (0,) * len(shape)
    return pl.BlockSpec(shape, lambda *_: zeros)


def held(x):
    return pltpu.with_memory_space_constraint(x, pltpu.VMEM), pl.BlockSpec(memory_space=pltpu.VMEM)


def copied(x, spec=None):
    return pltpu.with_memory_space_constraint(x, pltpu.HBM), spec or whole(x.shape)


def kernel(body, name, args, outs, us, grid=1, scratch=(), room=16):
    here = pl.BlockSpec(memory_space=pltpu.VMEM)
    return pl.pallas_call(
        body,
        grid=(grid,),
        in_specs=[spec for _, spec in args],
        out_specs=[here if spec is None else spec for _, _, spec in outs],
        out_shape=[
            (pltpu.VMEM if spec is None else pltpu.HBM)(shape, dtype)
            for shape, dtype, spec in outs
        ],
        scratch_shapes=scratch,
        cost_estimate=pl.CostEstimate(flops=int(us * 1e9), bytes_accessed=1000, transcendentals=0),
        compiler_params=pltpu.CompilerParams(vmem_limit_bytes=room * 2**20),
        name=name,
    )(*[x for x, _ in args])


def per_device(
    conv_value,
    conv_gate,
    taps,
    doc_ids,
    gn_gain,
    gn_shift,
    conv_out,
    residual,
    norm_gain,
    routes,
    route_weight,
    expert_gate,
    expert_up,
    expert_down,
    shared_gate,
    shared_up,
    shared_down,
):
    positions, channels = conv_value.shape
    tokens, model_width = residual.shape
    experts = expert_gate.shape[0] * lax.axis_size("sp") * lax.axis_size("tp")
    half = model_width // 2
    ids = doc_ids.reshape(1, positions)
    gain = gn_gain.reshape(1, channels)
    shift = gn_shift.reshape(1, channels)

    last = positions // HALO - 1
    tail = pl.BlockSpec((HALO, channels), lambda i: (last, 0))
    (packed,) = kernel(
        pack_kernel,
        "pack",
        [copied(conv_value, tail), copied(conv_gate, tail), copied(ids)],
        [((PACK, channels), BF16, None)],
        us=1,
    )
    halo = from_behind(packed, "sp", 1)
    (act,) = kernel(
        conv_kernel,
        "conv",
        [held(conv_value), held(conv_gate), held(taps), held(ids), held(gain), held(shift)],
        [((positions, channels), BF16, None)],
        us=4,
        scratch=[
            pltpu.VMEM((positions + 8, 128), F32),
            pltpu.VMEM((8, positions, 128), F32),
            pltpu.VMEM((positions, 128), F32),
        ],
    )
    keep, send = kernel(
        rim_kernel,
        "rim",
        [
            held(act),
            held(conv_value),
            held(conv_gate),
            held(taps),
            held(ids),
            held(halo),
            held(gain),
            held(shift),
        ],
        [((tokens, channels), BF16, None), ((tokens, channels), BF16, None)],
        us=1,
        scratch=[pltpu.VMEM((2 * HALO + 8, 128), F32), pltpu.VMEM((8, 2 * HALO, 128), F32)],
    )
    got = lax.ppermute(send, "tp", [(0, 1), (1, 0)])
    meta, pick = kernel(
        route_kernel,
        "route",
        [held(routes.T), held(route_weight.T)],
        [((8, tokens), F32, None), ((8 * experts, 2 * tokens), BF16, None)],
        us=2,
    )
    rows = (tokens, model_width)
    stream, normed, outgoing = kernel(
        spread_kernel,
        "spread",
        [
            held(keep),
            held(got),
            held(conv_out),
            held(residual),
            held(norm_gain.reshape(1, model_width)),
            held(pick),
        ],
        [(rows, BF16, whole(rows)), (rows, BF16, whole(rows)), ((8 * experts, half), BF16, None)],
        us=3,
    )

    exchange = functools.partial(
        lax.all_to_all, axis_name=("sp", "tp"), split_axis=0, concat_axis=0, tiled=True
    )
    arrived = exchange(outgoing.reshape(experts, 8, half)).reshape(8 * experts, half)
    piece = 128
    by_column = pl.BlockSpec((model_width, piece), lambda i: (0, i))
    (base,) = kernel(
        shared_kernel,
        "shared",
        [
            copied(normed),
            copied(stream),
            copied(shared_gate, by_column),
            copied(shared_up, by_column),
            copied(shared_down, pl.BlockSpec((piece, model_width), lambda i: (i, 0))),
        ],
        [(rows, F32, None)],
        us=8,
        grid=shared_gate.shape[1] // piece,
    )
    (result,) = kernel(
        expert_kernel,
        "expert",
        [held(arrived), held(expert_gate[0]), held(expert_up[0]), held(expert_down[0])],
        [((8 * experts, half), BF16, pl.BlockSpec((2 * experts, half), lambda i: (i, 0)))],
        us=5,
        grid=4,
    )
    returned = exchange(result.reshape(experts, 8, half)).reshape(8 * experts, half)
    (out,) = kernel(
        gather_kernel,
        "gather",
        [held(returned), held(meta), held(base)],
        [(rows, BF16, pl.BlockSpec((tokens, half), lambda i: (0, i)))],
        us=2,
        grid=2,
    )
    return out


def solution(mesh):
    return jax.shard_map(
        per_device,
        mesh=mesh,
        in_specs=(
            P("sp", "tp"),
            P("sp", "tp"),
            P(None, "tp"),
            P("sp"),
            P("tp"),
            P("tp"),
            P(),
            P(("sp", "tp"), None),
            P(),
            P(("sp", "tp"), None),
            P(("sp", "tp"), None),
            P(("sp", "tp"), None, None),
            P(("sp", "tp"), None, None),
            P(("sp", "tp"), None, None),
            P(),
            P(),
            P(),
        ),
        out_specs=P(("sp", "tp"), None),
        check_vma=False,
    )
```

```python
import functools

import jax
import jax.numpy as jnp
from jax import lax
from jax.experimental import pallas as pl
from jax.experimental.pallas import tpu as pltpu
from jax.sharding import PartitionSpec as P

GROUPS = 8
EPS = 1e-06
F32 = jnp.float32
BF16 = jnp.bfloat16
HALO = 32
PACK = 40


def from_behind(x, axis, by):
    peers = lax.axis_size(axis)
    pairs = [(i, (i + by) % peers) for i in range(peers)]
    return lax.ppermute(x, axis, pairs)


def glu_of(value, gate):
    wide = value.astype(F32) * jax.nn.sigmoid(gate.astype(F32))
    return wide.astype(BF16)


def pack_kernel(value, gate, ids, out):
    channels = value.shape[1]
    positions = ids.shape[1]
    out[0:HALO, :] = glu_of(value[...], gate[...])
    tail = ids[:, positions - 128 :].astype(F32)
    row = jnp.concatenate([tail, jnp.zeros((1, channels - 128), F32)], axis=1)
    out[HALO:, :] = jnp.broadcast_to(row, (PACK - HALO, channels)).astype(BF16)


def same_document(column, row, first, behind, width):
    shape = (column.shape[0], row.shape[1])
    t = lax.broadcasted_iota(jnp.int32, shape, 0) + first
    s = lax.broadcasted_iota(jnp.int32, shape, 1) - behind
    near = (column == row) & (s < t) & (s > t - width)
    ones = jnp.ones((shape[1], 128), BF16)
    return jnp.dot(near.astype(F32).astype(BF16), ones, preferred_element_type=F32)


def column_of(row):
    return jnp.transpose(jnp.broadcast_to(row, (8, row.shape[1])))[:, 0:1]


def normalized(fetch, deep, taps, gain, shift, lanes):
    width = taps.shape[0]
    total = jnp.zeros(deep.shape, F32)
    for i in range(width):
        term = taps[i : i + 1, lanes].astype(F32) * fetch(i)
        lag = width - 1 - i
        total = total + (jnp.where(deep >= lag, term, 0.0) if lag else term)
    mean = jnp.mean(total, axis=-1, keepdims=True)
    centered = total - mean
    var = jnp.mean(centered * centered, axis=-1, keepdims=True)
    v = centered * lax.rsqrt(var + EPS) * gain[:, lanes] + shift[:, lanes]
    return jax.nn.silu(v).astype(BF16)


def conv_kernel(value, gate, taps, ids, gain, shift, act, ext, moved, depth):
    positions, channels = value.shape
    width = taps.shape[0]
    own = ids[...].astype(F32)
    depth[...] = same_document(column_of(own), own, 0, 0, width)
    ext[positions:, :] = jnp.zeros((8, 128), F32)
    for c in range(channels // 128):
        lanes = slice(c * 128, c * 128 + 128)
        ext[0:positions, :] = glu_of(value[:, lanes], gate[:, lanes]).astype(F32)
        for r in range(1, 8):
            moved[r, :, :] = ext[pl.ds(r, positions), :]
        base = HALO
        while base < positions:
            rows = HALO if base == HALO else 2 * HALO

            def fetch(i, base=base, rows=rows):
                start = base - (width - 1) + i
                r = start % 8
                at = slice(start - r, start - r + rows)
                return ext[at, :] if r == 0 else moved[r, at, :]

            deep = depth[base : base + rows, :]
            act[base : base + rows, lanes] = normalized(fetch, deep, taps, gain, shift, lanes)
            base += rows


def rim_kernel(act, value, gate, taps, ids, halo, gain, shift, keep, send, ext, moved):
    channels = value.shape[1]
    rows = HALO
    width = taps.shape[0]
    tokens = keep.shape[0]
    mine = lax.axis_index("tp")
    own = ids[...].astype(F32)
    column = column_of(own)[0:rows]
    deep = same_document(column, own, 0, 0, width) + same_document(
        column, halo[HALO : HALO + 1, 0:128].astype(F32), 0, 128, width
    )
    at = pl.multiple_of(mine * tokens, tokens)
    keep[rows:, :] = act[pl.ds(at + rows, tokens - rows), :]
    at = pl.multiple_of((1 - mine) * tokens, tokens)
    send[rows:, :] = act[pl.ds(at + rows, tokens - rows), :]
    ext[2 * HALO :, :] = jnp.zeros((8, 128), F32)
    for c in range(channels // 128):
        lanes = slice(c * 128, c * 128 + 128)
        ext[0:HALO, :] = halo[0:HALO, lanes].astype(F32)
        ext[HALO : 2 * HALO, :] = glu_of(value[0:rows, lanes], gate[0:rows, lanes]).astype(F32)
        for r in range(1, 8):
            moved[r, :, :] = ext[pl.ds(r, 2 * HALO), :]

        def fetch(i):
            start = HALO - (width - 1) + i
            r = start % 8
            at = slice(start - r, start - r + rows)
            return ext[at, :] if r == 0 else moved[r, at, :]

        first = normalized(fetch, deep, taps, gain, shift, lanes)

        second = act[tokens : tokens + rows, lanes]
        keep[0:rows, lanes] = jnp.where(mine == 0, first, second)
        send[0:rows, lanes] = jnp.where(mine == 0, second, first)


def route_kernel(routes, weights, meta, pick):
    tokens = routes.shape[1]
    experts = pick.shape[0] // 8
    expert = lax.broadcasted_iota(jnp.int32, (experts, tokens), 0)
    hot = [(expert == routes[k : k + 1, :]).astype(F32) for k in range(2)]
    a = lax.broadcasted_iota(jnp.int32, (tokens, tokens), 0)
    b = lax.broadcasted_iota(jnp.int32, (tokens, tokens), 1)
    before = (a < b).astype(F32).astype(BF16)
    ahead = [jnp.dot(h.astype(BF16), before, preferred_element_type=F32) for h in hot]
    ahead[1] = ahead[1] + jnp.sum(hot[0], axis=1, keepdims=True)
    slot = [jnp.sum(h * c, axis=0, keepdims=True) for h, c in zip(hot, ahead)]
    target = [routes[k : k + 1, :].astype(F32) * 4.0 + slot[k] for k in range(2)]
    meta[...] = jnp.concatenate(
        target + [weights[0:1, :], weights[1:2, :], jnp.zeros((4, tokens), F32)], axis=0
    )
    r = lax.broadcasted_iota(jnp.int32, (8 * experts, tokens), 0)
    slots = ((r // 8) * 4 + r % 4).astype(F32)
    half = (r // 4) % 2
    chosen = (slots == target[0]) | (slots == target[1])
    for h in range(2):
        pick[:, h * tokens : (h + 1) * tokens] = (chosen & (half == h)).astype(F32).astype(BF16)


def spread_kernel(keep, got, conv_out, residual, norm_gain, pick, stream, normed, outgoing):
    tokens, half_in = keep.shape
    model_width = residual.shape[1]
    mine = lax.axis_index("tp")
    first = pl.multiple_of(mine * half_in, half_in)
    other = pl.multiple_of((1 - mine) * half_in, half_in)
    part = jnp.dot(keep[...], conv_out[pl.ds(first, half_in), :], preferred_element_type=F32)
    part = part + jnp.dot(got[...], conv_out[pl.ds(other, half_in), :], preferred_element_type=F32)
    rows = (residual[...].astype(F32) + part).astype(BF16)
    stream[...] = rows
    wide = rows.astype(F32)
    scale = lax.rsqrt(jnp.mean(wide * wide, axis=-1, keepdims=True) + EPS)
    ready = (wide * scale * norm_gain[...]).astype(BF16)
    normed[...] = ready
    mid = model_width // 2
    source = jnp.concatenate([ready[:, 0:mid], ready[:, mid:]], axis=0)
    outgoing[...] = jnp.dot(pick[...], source, preferred_element_type=F32).astype(BF16)


def expert_kernel(x, gate, up, down, out, rows, done, sems):
    total, half = x.shape
    quads = total // 16
    piece = 256

    def low(width):
        return lax.broadcasted_iota(jnp.int32, (quads, 8, width), 1) < 4

    for at in range(0, half, piece):
        wide = x[:, at : at + piece].astype(F32).reshape(quads, 2, 8, piece)
        a, b = wide[:, 0], wide[:, 1]
        top = jnp.where(low(piece), a, pltpu.roll(b, 4, 1))
        bottom = jnp.where(low(piece), pltpu.roll(a, 4, 1), b)
        rows[:, at : at + piece] = top.reshape(quads * 8, piece).astype(BF16)
        rows[:, half + at : half + at + piece] = bottom.reshape(quads * 8, piece).astype(BF16)
    g = jnp.dot(rows[...], gate[...], preferred_element_type=F32)
    u = jnp.dot(rows[...], up[...], preferred_element_type=F32)
    hidden = (jax.nn.silu(g) * u).astype(BF16)
    copies = []
    for n, at in enumerate(range(0, half, piece)):
        left = jnp.dot(hidden, down[:, at : at + piece], preferred_element_type=F32)
        right = jnp.dot(hidden, down[:, half + at : half + at + piece], preferred_element_type=F32)
        left = left.reshape(quads, 8, piece)
        right = right.reshape(quads, 8, piece)
        first = jnp.where(low(piece), left, pltpu.roll(right, 4, 1))
        second = jnp.where(low(piece), pltpu.roll(left, 4, 1), right)
        done[n] = jnp.stack([first, second], axis=1).reshape(total, piece).astype(BF16)
        copies.append(pltpu.make_async_copy(done.at[n], out.at[:, at : at + piece], sems.at[n]))
        copies[-1].start()
    for copy in copies:
        copy.wait()


def shared_kernel(normed, stream, gate, up, down, out):
    rows = normed[...]
    g = jnp.dot(rows, gate[...], preferred_element_type=F32)
    u = jnp.dot(rows, up[...], preferred_element_type=F32)
    hidden = (jax.nn.silu(g) * u).astype(BF16)
    part = jnp.dot(hidden, down[...], preferred_element_type=F32)

    @pl.when(pl.program_id(0) == 0)
    def _():
        out[...] = stream[...].astype(F32) + part

    @pl.when(pl.program_id(0) > 0)
    def _():
        out[...] += part


def gather_kernel(returned, meta, base, out, ready, sems):
    rows, half = returned.shape
    tokens = base.shape[0]
    piece = 256
    columns = jnp.transpose(meta[...])
    r = lax.broadcasted_iota(jnp.int32, (tokens, rows), 1)
    slots = ((r // 8) * 4 + r % 4).astype(F32)
    weight = jnp.where(
        slots == columns[:, 0:1],
        columns[:, 2:3],
        jnp.where(slots == columns[:, 1:2], columns[:, 3:4], 0.0),
    )
    lower = (r // 4) % 2 == 0
    weights = jnp.concatenate(
        [jnp.where(lower, weight, 0.0), jnp.where(lower, 0.0, weight)], axis=0
    ).astype(BF16)
    copies = []
    for n, at in enumerate(range(0, half, piece)):
        routed = jnp.dot(weights, returned[:, at : at + piece], preferred_element_type=F32)
        for h in range(2):
            k = 2 * n + h
            here = slice(h * half + at, h * half + at + piece)
            ready[k] = (base[:, here] + routed[h * tokens : (h + 1) * tokens, :]).astype(BF16)
            copies.append(pltpu.make_async_copy(ready.at[k], out.at[:, here], sems.at[k]))
            copies[-1].start()
    for copy in copies:
        copy.wait()


def whole(shape):
    zeros = (0,) * len(shape)
    return pl.BlockSpec(shape, lambda *_: zeros)


def held(x):
    return pltpu.with_memory_space_constraint(x, pltpu.VMEM), pl.BlockSpec(memory_space=pltpu.VMEM)


def copied(x, spec=None):
    return pltpu.with_memory_space_constraint(x, pltpu.HBM), spec or whole(x.shape)


def kernel(body, name, args, outs, us, grid=1, scratch=(), room=16):
    here = pl.BlockSpec(memory_space=pltpu.VMEM)
    return pl.pallas_call(
        body,
        grid=(grid,),
        in_specs=[spec for _, spec in args],
        out_specs=[here if spec is None else spec for _, _, spec in outs],
        out_shape=[
            (pltpu.VMEM if spec is None else pltpu.HBM)(shape, dtype)
            for shape, dtype, spec in outs
        ],
        scratch_shapes=scratch,
        cost_estimate=pl.CostEstimate(flops=int(us * 1e9), bytes_accessed=1000, transcendentals=0),
        compiler_params=pltpu.CompilerParams(vmem_limit_bytes=room * 2**20),
        name=name,
    )(*[x for x, _ in args])


def per_device(
    conv_value,
    conv_gate,
    taps,
    doc_ids,
    gn_gain,
    gn_shift,
    conv_out,
    residual,
    norm_gain,
    routes,
    route_weight,
    expert_gate,
    expert_up,
    expert_down,
    shared_gate,
    shared_up,
    shared_down,
):
    positions, channels = conv_value.shape
    tokens, model_width = residual.shape
    experts = expert_gate.shape[0] * lax.axis_size("sp") * lax.axis_size("tp")
    half = model_width // 2
    ids = doc_ids.reshape(1, positions)
    gain = gn_gain.reshape(1, channels)
    shift = gn_shift.reshape(1, channels)

    last = positions // HALO - 1
    tail = pl.BlockSpec((HALO, channels), lambda i: (last, 0))
    (packed,) = kernel(
        pack_kernel,
        "pack",
        [copied(conv_value, tail), copied(conv_gate, tail), copied(ids)],
        [((PACK, channels), BF16, None)],
        us=1,
    )
    halo = from_behind(packed, "sp", 1)
    (act,) = kernel(
        conv_kernel,
        "conv",
        [held(conv_value), held(conv_gate), held(taps), held(ids), held(gain), held(shift)],
        [((positions, channels), BF16, None)],
        us=4,
        scratch=[
            pltpu.VMEM((positions + 8, 128), F32),
            pltpu.VMEM((8, positions, 128), F32),
            pltpu.VMEM((positions, 128), F32),
        ],
    )
    keep, send = kernel(
        rim_kernel,
        "rim",
        [
            held(act),
            held(conv_value),
            held(conv_gate),
            held(taps),
            held(ids),
            held(halo),
            held(gain),
            held(shift),
        ],
        [((tokens, channels), BF16, None), ((tokens, channels), BF16, None)],
        us=0.3,
        scratch=[pltpu.VMEM((2 * HALO + 8, 128), F32), pltpu.VMEM((8, 2 * HALO, 128), F32)],
    )
    got = lax.ppermute(send, "tp", [(0, 1), (1, 0)])
    meta, pick = kernel(
        route_kernel,
        "route",
        [held(routes.T), held(route_weight.T)],
        [((8, tokens), F32, None), ((8 * experts, 2 * tokens), BF16, None)],
        us=0.3,
    )
    rows = (tokens, model_width)
    stream, normed, outgoing = kernel(
        spread_kernel,
        "spread",
        [
            held(keep),
            held(got),
            held(conv_out),
            held(residual),
            held(norm_gain.reshape(1, model_width)),
            held(pick),
        ],
        [(rows, BF16, whole(rows)), (rows, BF16, whole(rows)), ((8 * experts, half), BF16, None)],
        us=3,
    )

    exchange = functools.partial(
        lax.all_to_all, axis_name=("sp", "tp"), split_axis=0, concat_axis=0, tiled=True
    )
    arrived = exchange(outgoing.reshape(experts, 8, half)).reshape(8 * experts, half)
    piece = 128
    by_column = pl.BlockSpec((model_width, piece), lambda i: (0, i))
    (base,) = kernel(
        shared_kernel,
        "shared",
        [
            copied(normed),
            copied(stream),
            copied(shared_gate, by_column),
            copied(shared_up, by_column),
            copied(shared_down, pl.BlockSpec((piece, model_width), lambda i: (i, 0))),
        ],
        [(rows, F32, None)],
        us=8,
        grid=shared_gate.shape[1] // piece,
    )
    outside = pl.BlockSpec(memory_space=pltpu.HBM)
    (result,) = kernel(
        expert_kernel,
        "expert",
        [held(arrived), held(expert_gate[0]), held(expert_up[0]), held(expert_down[0])],
        [((8 * experts, half), BF16, outside)],
        us=5,
        scratch=[
            pltpu.VMEM((4 * experts, model_width), BF16),
            pltpu.VMEM((half // 256, 8 * experts, 256), BF16),
            pltpu.SemaphoreType.DMA((half // 256,)),
        ],
    )
    returned = exchange(result.reshape(experts, 8, half)).reshape(8 * experts, half)
    (out,) = kernel(
        gather_kernel,
        "gather",
        [held(returned), held(meta), held(base)],
        [(rows, BF16, outside)],
        us=2,
        scratch=[
            pltpu.VMEM((model_width // 256, tokens, 256), BF16),
            pltpu.SemaphoreType.DMA((model_width // 256,)),
        ],
    )
    return out


def solution(mesh):
    return jax.shard_map(
        per_device,
        mesh=mesh,
        in_specs=(
            P("sp", "tp"),
            P("sp", "tp"),
            P(None, "tp"),
            P("sp"),
            P("tp"),
            P("tp"),
            P(),
            P(("sp", "tp"), None),
            P(),
            P(("sp", "tp"), None),
            P(("sp", "tp"), None),
            P(("sp", "tp"), None, None),
            P(("sp", "tp"), None, None),
            P(("sp", "tp"), None, None),
            P(),
            P(),
            P(),
        ),
        out_specs=P(("sp", "tp"), None),
        check_vma=False,
    )
```

```python
import functools

import jax
import jax.numpy as jnp
from jax import lax
from jax.experimental import pallas as pl
from jax.experimental.pallas import tpu as pltpu
from jax.sharding import PartitionSpec as P

GROUPS = 8
EPS = 1e-06
F32 = jnp.float32
BF16 = jnp.bfloat16
HALO = 32


def from_behind(x, axis, by):
    peers = lax.axis_size(axis)
    pairs = [(i, (i + by) % peers) for i in range(peers)]
    return lax.ppermute(x, axis, pairs)


def glu_of(value, gate):
    wide = value.astype(F32) * jax.nn.sigmoid(gate.astype(F32))
    return wide.astype(BF16)


def pack_kernel(value, gate, ids, out):
    channels = value.shape[1]
    positions = ids.shape[1]
    tail = ids[:, positions - 128 :].astype(F32)
    row = jnp.concatenate([tail, jnp.zeros((1, channels - 128), F32)], axis=1)
    first = lax.broadcasted_iota(jnp.int32, (HALO, channels), 0) == 0
    rows = glu_of(value[...], gate[...]).astype(F32)
    out[...] = jnp.where(first, row, rows).astype(BF16)


def same_document(column, row, first, behind, width):
    shape = (column.shape[0], row.shape[1])
    t = lax.broadcasted_iota(jnp.int32, shape, 0) + first
    s = lax.broadcasted_iota(jnp.int32, shape, 1) - behind
    near = (column == row) & (s < t) & (s > t - width)
    ones = jnp.ones((shape[1], 128), BF16)
    return jnp.dot(near.astype(F32).astype(BF16), ones, preferred_element_type=F32)


def column_of(row):
    return jnp.transpose(jnp.broadcast_to(row, (8, row.shape[1])))[:, 0:1]


def normalized(fetch, deep, taps, gain, shift, lanes):
    width = taps.shape[0]
    total = jnp.zeros(deep.shape, F32)
    for i in range(width):
        term = taps[i : i + 1, lanes].astype(F32) * fetch(i)
        lag = width - 1 - i
        total = total + (jnp.where(deep >= lag, term, 0.0) if lag else term)
    mean = jnp.mean(total, axis=-1, keepdims=True)
    centered = total - mean
    var = jnp.mean(centered * centered, axis=-1, keepdims=True)
    v = centered * lax.rsqrt(var + EPS) * gain[:, lanes] + shift[:, lanes]
    return jax.nn.silu(v).astype(BF16)


def conv_kernel(value, gate, taps, ids, gain, shift, act, ext, moved, depth):
    positions, channels = value.shape
    width = taps.shape[0]
    own = ids[...].astype(F32)
    depth[...] = same_document(column_of(own), own, 0, 0, width)
    ext[positions:, :] = jnp.zeros((8, 128), F32)
    for c in range(channels // 128):
        lanes = slice(c * 128, c * 128 + 128)
        ext[0:positions, :] = glu_of(value[:, lanes], gate[:, lanes]).astype(F32)
        for r in range(1, 8):
            moved[r, :, :] = ext[pl.ds(r, positions), :]
        base = HALO
        while base < positions:
            rows = HALO if base == HALO else 2 * HALO

            def fetch(i, base=base, rows=rows):
                start = base - (width - 1) + i
                r = start % 8
                at = slice(start - r, start - r + rows)
                return ext[at, :] if r == 0 else moved[r, at, :]

            deep = depth[base : base + rows, :]
            act[base : base + rows, lanes] = normalized(fetch, deep, taps, gain, shift, lanes)
            base += rows


def rim_kernel(act, value, gate, taps, ids, halo, gain, shift, keep, send, ext, moved):
    channels = value.shape[1]
    rows = HALO
    width = taps.shape[0]
    tokens = keep.shape[0]
    mine = lax.axis_index("tp")
    own = ids[...].astype(F32)
    column = column_of(own)[0:rows]
    deep = same_document(column, own, 0, 0, width) + same_document(
        column, halo[0:1, 0:128].astype(F32), 0, 128, width
    )
    at = pl.multiple_of(mine * tokens, tokens)
    keep[rows:, :] = act[pl.ds(at + rows, tokens - rows), :]
    at = pl.multiple_of((1 - mine) * tokens, tokens)
    send[rows:, :] = act[pl.ds(at + rows, tokens - rows), :]
    ext[2 * HALO :, :] = jnp.zeros((8, 128), F32)
    for c in range(channels // 128):
        lanes = slice(c * 128, c * 128 + 128)
        ext[0:HALO, :] = halo[0:HALO, lanes].astype(F32)
        ext[HALO : 2 * HALO, :] = glu_of(value[0:rows, lanes], gate[0:rows, lanes]).astype(F32)
        for r in range(1, 8):
            moved[r, :, :] = ext[pl.ds(r, 2 * HALO), :]

        def fetch(i):
            start = HALO - (width - 1) + i
            r = start % 8
            at = slice(start - r, start - r + rows)
            return ext[at, :] if r == 0 else moved[r, at, :]

        first = normalized(fetch, deep, taps, gain, shift, lanes)

        second = act[tokens : tokens + rows, lanes]
        keep[0:rows, lanes] = jnp.where(mine == 0, first, second)
        send[0:rows, lanes] = jnp.where(mine == 0, second, first)


def route_kernel(routes, weights, meta, pick):
    tokens = routes.shape[1]
    experts = pick.shape[0] // 8
    expert = lax.broadcasted_iota(jnp.int32, (experts, tokens), 0)
    hot = [(expert == routes[k : k + 1, :]).astype(F32) for k in range(2)]
    a = lax.broadcasted_iota(jnp.int32, (tokens, tokens), 0)
    b = lax.broadcasted_iota(jnp.int32, (tokens, tokens), 1)
    before = (a < b).astype(F32).astype(BF16)
    ahead = [jnp.dot(h.astype(BF16), before, preferred_element_type=F32) for h in hot]
    ahead[1] = ahead[1] + jnp.sum(hot[0], axis=1, keepdims=True)
    slot = [jnp.sum(h * c, axis=0, keepdims=True) for h, c in zip(hot, ahead)]
    target = [routes[k : k + 1, :].astype(F32) * 4.0 + slot[k] for k in range(2)]
    meta[...] = jnp.concatenate(
        target + [weights[0:1, :], weights[1:2, :], jnp.zeros((4, tokens), F32)], axis=0
    )
    r = lax.broadcasted_iota(jnp.int32, (8 * experts, tokens), 0)
    slots = ((r // 8) * 4 + r % 4).astype(F32)
    half = (r // 4) % 2
    chosen = (slots == target[0]) | (slots == target[1])
    for h in range(2):
        pick[:, h * tokens : (h + 1) * tokens] = (chosen & (half == h)).astype(F32).astype(BF16)


def spread_kernel(keep, got, conv_out, residual, norm_gain, pick, stream, normed, outgoing, left, right, sems):
    tokens, half_in = keep.shape
    model_width = residual.shape[1]
    mine = lax.axis_index("tp")
    near = pl.multiple_of(mine * half_in, half_in)
    other = pl.multiple_of((1 - mine) * half_in, half_in)
    part = jnp.dot(keep[...], conv_out[pl.ds(near, half_in), :], preferred_element_type=F32)
    part = part + jnp.dot(got[...], conv_out[pl.ds(other, half_in), :], preferred_element_type=F32)
    rows = (residual[...].astype(F32) + part).astype(BF16)
    left[...] = rows
    first = pltpu.make_async_copy(left, stream, sems.at[0])
    first.start()
    wide = rows.astype(F32)
    scale = lax.rsqrt(jnp.mean(wide * wide, axis=-1, keepdims=True) + EPS)
    ready = (wide * scale * norm_gain[...]).astype(BF16)
    right[...] = ready
    second = pltpu.make_async_copy(right, normed, sems.at[1])
    second.start()
    mid = model_width // 2
    source = jnp.concatenate([ready[:, 0:mid], ready[:, mid:]], axis=0)
    outgoing[...] = jnp.dot(pick[...], source, preferred_element_type=F32).astype(BF16)
    first.wait()
    second.wait()


def expert_kernel(x, gate, up, down, out, rows, done, sems):
    total, half = x.shape
    quads = total // 16
    piece = 256

    def low(width):
        return lax.broadcasted_iota(jnp.int32, (quads, 8, width), 1) < 4

    for at in range(0, half, piece):
        wide = x[:, at : at + piece].astype(F32).reshape(quads, 2, 8, piece)
        a, b = wide[:, 0], wide[:, 1]
        top = jnp.where(low(piece), a, pltpu.roll(b, 4, 1))
        bottom = jnp.where(low(piece), pltpu.roll(a, 4, 1), b)
        rows[:, at : at + piece] = top.reshape(quads * 8, piece).astype(BF16)
        rows[:, half + at : half + at + piece] = bottom.reshape(quads * 8, piece).astype(BF16)
    g = jnp.dot(rows[...], gate[...], preferred_element_type=F32)
    u = jnp.dot(rows[...], up[...], preferred_element_type=F32)
    hidden = (jax.nn.silu(g) * u).astype(BF16)
    copies = []
    for n, at in enumerate(range(0, half, piece)):
        left = jnp.dot(hidden, down[:, at : at + piece], preferred_element_type=F32)
        right = jnp.dot(hidden, down[:, half + at : half + at + piece], preferred_element_type=F32)
        left = left.reshape(quads, 8, piece)
        right = right.reshape(quads, 8, piece)
        first = jnp.where(low(piece), left, pltpu.roll(right, 4, 1))
        second = jnp.where(low(piece), pltpu.roll(left, 4, 1), right)
        done[n] = jnp.stack([first, second], axis=1).reshape(total, piece).astype(BF16)
        copies.append(pltpu.make_async_copy(done.at[n], out.at[:, at : at + piece], sems.at[n]))
        copies[-1].start()
    for copy in copies:
        copy.wait()


def shared_kernel(normed, stream, gate, up, down, out):
    rows = normed[...]
    g = jnp.dot(rows, gate[...], preferred_element_type=F32)
    u = jnp.dot(rows, up[...], preferred_element_type=F32)
    hidden = (jax.nn.silu(g) * u).astype(BF16)
    part = jnp.dot(hidden, down[...], preferred_element_type=F32)

    @pl.when(pl.program_id(0) == 0)
    def _():
        out[...] = stream[...].astype(F32) + part

    @pl.when(pl.program_id(0) > 0)
    def _():
        out[...] += part


def gather_kernel(returned, meta, base, out, ready, sems):
    rows, half = returned.shape
    tokens = base.shape[0]
    piece = 256
    columns = jnp.transpose(meta[...])
    r = lax.broadcasted_iota(jnp.int32, (tokens, rows), 1)
    slots = ((r // 8) * 4 + r % 4).astype(F32)
    weight = jnp.where(
        slots == columns[:, 0:1],
        columns[:, 2:3],
        jnp.where(slots == columns[:, 1:2], columns[:, 3:4], 0.0),
    )
    lower = (r // 4) % 2 == 0
    weights = jnp.concatenate(
        [jnp.where(lower, weight, 0.0), jnp.where(lower, 0.0, weight)], axis=0
    ).astype(BF16)
    copies = []
    for n, at in enumerate(range(0, half, piece)):
        routed = jnp.dot(weights, returned[:, at : at + piece], preferred_element_type=F32)
        for h in range(2):
            k = 2 * n + h
            here = slice(h * half + at, h * half + at + piece)
            ready[k] = (base[:, here] + routed[h * tokens : (h + 1) * tokens, :]).astype(BF16)
            copies.append(pltpu.make_async_copy(ready.at[k], out.at[:, here], sems.at[k]))
            copies[-1].start()
    for copy in copies:
        copy.wait()


def whole(shape):
    zeros = (0,) * len(shape)
    return pl.BlockSpec(shape, lambda *_: zeros)


def held(x):
    return pltpu.with_memory_space_constraint(x, pltpu.VMEM), pl.BlockSpec(memory_space=pltpu.VMEM)


def copied(x, spec=None):
    return pltpu.with_memory_space_constraint(x, pltpu.HBM), spec or whole(x.shape)


def kernel(body, name, args, outs, us, grid=1, scratch=(), room=16):
    here = pl.BlockSpec(memory_space=pltpu.VMEM)
    return pl.pallas_call(
        body,
        grid=(grid,),
        in_specs=[spec for _, spec in args],
        out_specs=[here if spec is None else spec for _, _, spec in outs],
        out_shape=[
            (pltpu.VMEM if spec is None else pltpu.HBM)(shape, dtype)
            for shape, dtype, spec in outs
        ],
        scratch_shapes=scratch,
        cost_estimate=pl.CostEstimate(flops=int(us * 1e9), bytes_accessed=1000, transcendentals=0),
        compiler_params=pltpu.CompilerParams(vmem_limit_bytes=room * 2**20),
        name=name,
    )(*[x for x, _ in args])


def per_device(
    conv_value,
    conv_gate,
    taps,
    doc_ids,
    gn_gain,
    gn_shift,
    conv_out,
    residual,
    norm_gain,
    routes,
    route_weight,
    expert_gate,
    expert_up,
    expert_down,
    shared_gate,
    shared_up,
    shared_down,
):
    positions, channels = conv_value.shape
    tokens, model_width = residual.shape
    experts = expert_gate.shape[0] * lax.axis_size("sp") * lax.axis_size("tp")
    half = model_width // 2
    ids = doc_ids.reshape(1, positions)
    gain = gn_gain.reshape(1, channels)
    shift = gn_shift.reshape(1, channels)

    last = positions // HALO - 1
    tail = pl.BlockSpec((HALO, channels), lambda i: (last, 0))
    (packed,) = kernel(
        pack_kernel,
        "pack",
        [copied(conv_value, tail), copied(conv_gate, tail), copied(ids)],
        [((HALO, channels), BF16, None)],
        us=1,
    )
    halo = from_behind(packed, "sp", 1)
    (act,) = kernel(
        conv_kernel,
        "conv",
        [held(conv_value), held(conv_gate), held(taps), held(ids), held(gain), held(shift)],
        [((positions, channels), BF16, None)],
        us=4,
        scratch=[
            pltpu.VMEM((positions + 8, 128), F32),
            pltpu.VMEM((8, positions, 128), F32),
            pltpu.VMEM((positions, 128), F32),
        ],
    )
    keep, send = kernel(
        rim_kernel,
        "rim",
        [
            held(act),
            held(conv_value),
            held(conv_gate),
            held(taps),
            held(ids),
            held(halo),
            held(gain),
            held(shift),
        ],
        [((tokens, channels), BF16, None), ((tokens, channels), BF16, None)],
        us=0.3,
        scratch=[pltpu.VMEM((2 * HALO + 8, 128), F32), pltpu.VMEM((8, 2 * HALO, 128), F32)],
    )
    got = lax.ppermute(send, "tp", [(0, 1), (1, 0)])
    meta, pick = kernel(
        route_kernel,
        "route",
        [held(routes.T), held(route_weight.T)],
        [((8, tokens), F32, None), ((8 * experts, 2 * tokens), BF16, None)],
        us=0.3,
    )
    rows = (tokens, model_width)
    outside = pl.BlockSpec(memory_space=pltpu.HBM)
    stream, normed, outgoing = kernel(
        spread_kernel,
        "spread",
        [
            held(keep),
            held(got),
            held(conv_out),
            held(residual),
            held(norm_gain.reshape(1, model_width)),
            held(pick),
        ],
        [(rows, BF16, outside), (rows, BF16, outside), ((8 * experts, half), BF16, None)],
        us=3,
        scratch=[pltpu.VMEM(rows, BF16), pltpu.VMEM(rows, BF16), pltpu.SemaphoreType.DMA((2,))],
    )

    exchange = functools.partial(
        lax.all_to_all, axis_name=("sp", "tp"), split_axis=0, concat_axis=0, tiled=True
    )
    arrived = exchange(outgoing.reshape(experts, 8, half)).reshape(8 * experts, half)
    piece = 128
    by_column = pl.BlockSpec((model_width, piece), lambda i: (0, i))
    (base,) = kernel(
        shared_kernel,
        "shared",
        [
            copied(normed),
            copied(stream),
            copied(shared_gate, by_column),
            copied(shared_up, by_column),
            copied(shared_down, pl.BlockSpec((piece, model_width), lambda i: (i, 0))),
        ],
        [(rows, F32, None)],
        us=8,
        grid=shared_gate.shape[1] // piece,
    )
    (result,) = kernel(
        expert_kernel,
        "expert",
        [held(arrived), held(expert_gate[0]), held(expert_up[0]), held(expert_down[0])],
        [((8 * experts, half), BF16, outside)],
        us=5,
        scratch=[
            pltpu.VMEM((4 * experts, model_width), BF16),
            pltpu.VMEM((half // 256, 8 * experts, 256), BF16),
            pltpu.SemaphoreType.DMA((half // 256,)),
        ],
    )
    returned = exchange(result.reshape(experts, 8, half)).reshape(8 * experts, half)
    (out,) = kernel(
        gather_kernel,
        "gather",
        [held(returned), held(meta), held(base)],
        [(rows, BF16, outside)],
        us=2,
        scratch=[
            pltpu.VMEM((model_width // 256, tokens, 256), BF16),
            pltpu.SemaphoreType.DMA((model_width // 256,)),
        ],
    )
    return out


def solution(mesh):
    return jax.shard_map(
        per_device,
        mesh=mesh,
        in_specs=(
            P("sp", "tp"),
            P("sp", "tp"),
            P(None, "tp"),
            P("sp"),
            P("tp"),
            P("tp"),
            P(),
            P(("sp", "tp"), None),
            P(),
            P(("sp", "tp"), None),
            P(("sp", "tp"), None),
            P(("sp", "tp"), None, None),
            P(("sp", "tp"), None, None),
            P(("sp", "tp"), None, None),
            P(),
            P(),
            P(),
        ),
        out_specs=P(("sp", "tp"), None),
        check_vma=False,
    )
```

```python
import functools

import jax
import jax.numpy as jnp
from jax import lax
from jax.experimental import pallas as pl
from jax.experimental.pallas import tpu as pltpu
from jax.sharding import PartitionSpec as P

GROUPS = 8
EPS = 1e-06
F32 = jnp.float32
BF16 = jnp.bfloat16
HALO = 32


def from_behind(x, axis, by):
    peers = lax.axis_size(axis)
    pairs = [(i, (i + by) % peers) for i in range(peers)]
    return lax.ppermute(x, axis, pairs)


def glu_of(value, gate):
    wide = value.astype(F32) * jax.nn.sigmoid(gate.astype(F32))
    return wide.astype(BF16)


def pack_kernel(value, gate, ids, out):
    channels = value.shape[1]
    positions = ids.shape[1]
    tail = ids[:, positions - 128 :].astype(F32)
    row = jnp.concatenate([tail, jnp.zeros((1, channels - 128), F32)], axis=1)
    first = lax.broadcasted_iota(jnp.int32, (HALO, channels), 0) == 0
    rows = glu_of(value[...], gate[...]).astype(F32)
    out[...] = jnp.where(first, row, rows).astype(BF16)


def same_document(column, row, first, behind, width):
    shape = (column.shape[0], row.shape[1])
    t = lax.broadcasted_iota(jnp.int32, shape, 0) + first
    s = lax.broadcasted_iota(jnp.int32, shape, 1) - behind
    near = (column == row) & (s < t) & (s > t - width)
    ones = jnp.ones((shape[1], 128), BF16)
    return jnp.dot(near.astype(F32).astype(BF16), ones, preferred_element_type=F32)


def column_of(row):
    return jnp.transpose(jnp.broadcast_to(row, (8, row.shape[1])))[:, 0:1]


def normalized(fetch, deep, taps, gain, shift, lanes):
    width = taps.shape[0]
    total = jnp.zeros(deep.shape, F32)
    for i in range(width):
        term = taps[i : i + 1, lanes].astype(F32) * fetch(i)
        lag = width - 1 - i
        total = total + (jnp.where(deep >= lag, term, 0.0) if lag else term)
    mean = jnp.mean(total, axis=-1, keepdims=True)
    centered = total - mean
    var = jnp.mean(centered * centered, axis=-1, keepdims=True)
    v = centered * lax.rsqrt(var + EPS) * gain[:, lanes] + shift[:, lanes]
    return jax.nn.silu(v).astype(BF16)


def conv_kernel(value, gate, taps, ids, gain, shift, act, ext, moved, depth):
    positions, channels = value.shape
    width = taps.shape[0]
    own = ids[...].astype(F32)
    depth[...] = same_document(column_of(own), own, 0, 0, width)
    ext[positions:, :] = jnp.zeros((8, 128), F32)
    for c in range(channels // 128):
        lanes = slice(c * 128, c * 128 + 128)
        ext[0:positions, :] = glu_of(value[:, lanes], gate[:, lanes]).astype(F32)
        for r in range(1, 8):
            moved[r, :, :] = ext[pl.ds(r, positions), :]
        base = HALO
        while base < positions:
            rows = HALO if base == HALO else 2 * HALO

            def fetch(i, base=base, rows=rows):
                start = base - (width - 1) + i
                r = start % 8
                at = slice(start - r, start - r + rows)
                return ext[at, :] if r == 0 else moved[r, at, :]

            deep = depth[base : base + rows, :]
            act[base : base + rows, lanes] = normalized(fetch, deep, taps, gain, shift, lanes)
            base += rows


def rim_kernel(act, value, gate, taps, ids, halo, gain, shift, keep, send, ext, moved):
    channels = value.shape[1]
    rows = HALO
    width = taps.shape[0]
    tokens = keep.shape[0]
    mine = lax.axis_index("tp")
    own = ids[...].astype(F32)
    column = column_of(own)[0:rows]
    deep = same_document(column, own, 0, 0, width) + same_document(
        column, halo[0:1, 0:128].astype(F32), 0, 128, width
    )
    at = pl.multiple_of(mine * tokens, tokens)
    keep[rows:, :] = act[pl.ds(at + rows, tokens - rows), :]
    at = pl.multiple_of((1 - mine) * tokens, tokens)
    send[rows:, :] = act[pl.ds(at + rows, tokens - rows), :]
    ext[2 * HALO :, :] = jnp.zeros((8, 128), F32)
    for c in range(channels // 128):
        lanes = slice(c * 128, c * 128 + 128)
        ext[0:HALO, :] = halo[0:HALO, lanes].astype(F32)
        ext[HALO : 2 * HALO, :] = glu_of(value[0:rows, lanes], gate[0:rows, lanes]).astype(F32)
        for r in range(1, 8):
            moved[r, :, :] = ext[pl.ds(r, 2 * HALO), :]

        def fetch(i):
            start = HALO - (width - 1) + i
            r = start % 8
            at = slice(start - r, start - r + rows)
            return ext[at, :] if r == 0 else moved[r, at, :]

        first = normalized(fetch, deep, taps, gain, shift, lanes)

        second = act[tokens : tokens + rows, lanes]
        keep[0:rows, lanes] = jnp.where(mine == 0, first, second)
        send[0:rows, lanes] = jnp.where(mine == 0, second, first)


def route_kernel(routes, weights, keep, conv_out, residual, meta, pick, part):
    half_in = keep.shape[1]
    near = pl.multiple_of(lax.axis_index("tp") * half_in, half_in)
    part[...] = residual[...].astype(F32) + jnp.dot(
        keep[...], conv_out[pl.ds(near, half_in), :], preferred_element_type=F32
    )
    tokens = routes.shape[1]
    experts = pick.shape[0] // 8
    expert = lax.broadcasted_iota(jnp.int32, (experts, tokens), 0)
    hot = [(expert == routes[k : k + 1, :]).astype(F32) for k in range(2)]
    a = lax.broadcasted_iota(jnp.int32, (tokens, tokens), 0)
    b = lax.broadcasted_iota(jnp.int32, (tokens, tokens), 1)
    before = (a < b).astype(F32).astype(BF16)
    ahead = [jnp.dot(h.astype(BF16), before, preferred_element_type=F32) for h in hot]
    ahead[1] = ahead[1] + jnp.sum(hot[0], axis=1, keepdims=True)
    slot = [jnp.sum(h * c, axis=0, keepdims=True) for h, c in zip(hot, ahead)]
    target = [routes[k : k + 1, :].astype(F32) * 4.0 + slot[k] for k in range(2)]
    meta[...] = jnp.concatenate(
        target + [weights[0:1, :], weights[1:2, :], jnp.zeros((4, tokens), F32)], axis=0
    )
    r = lax.broadcasted_iota(jnp.int32, (8 * experts, tokens), 0)
    slots = ((r // 8) * 4 + r % 4).astype(F32)
    half = (r // 4) % 2
    chosen = (slots == target[0]) | (slots == target[1])
    for h in range(2):
        pick[:, h * tokens : (h + 1) * tokens] = (chosen & (half == h)).astype(F32).astype(BF16)


def spread_kernel(got, conv_out, part, norm_gain, pick, stream, normed, outgoing, left, right, sems):
    half_in = got.shape[1]
    model_width = part.shape[1]
    other = pl.multiple_of((1 - lax.axis_index("tp")) * half_in, half_in)
    rows = jnp.dot(got[...], conv_out[pl.ds(other, half_in), :], preferred_element_type=F32)
    rows = (part[...] + rows).astype(BF16)
    left[...] = rows
    first = pltpu.make_async_copy(left, stream, sems.at[0])
    first.start()
    wide = rows.astype(F32)
    scale = lax.rsqrt(jnp.mean(wide * wide, axis=-1, keepdims=True) + EPS)
    ready = (wide * scale * norm_gain[...]).astype(BF16)
    right[...] = ready
    second = pltpu.make_async_copy(right, normed, sems.at[1])
    second.start()
    mid = model_width // 2
    source = jnp.concatenate([ready[:, 0:mid], ready[:, mid:]], axis=0)
    outgoing[...] = jnp.dot(pick[...], source, preferred_element_type=F32).astype(BF16)
    first.wait()
    second.wait()


def expert_kernel(x, gate, up, down, out, rows, done, sems):
    total, half = x.shape
    quads = total // 16
    piece = 256

    def low(width):
        return lax.broadcasted_iota(jnp.int32, (quads, 8, width), 1) < 4

    for at in range(0, half, piece):
        wide = x[:, at : at + piece].astype(F32).reshape(quads, 2, 8, piece)
        a, b = wide[:, 0], wide[:, 1]
        top = jnp.where(low(piece), a, pltpu.roll(b, 4, 1))
        bottom = jnp.where(low(piece), pltpu.roll(a, 4, 1), b)
        rows[:, at : at + piece] = top.reshape(quads * 8, piece).astype(BF16)
        rows[:, half + at : half + at + piece] = bottom.reshape(quads * 8, piece).astype(BF16)
    g = jnp.dot(rows[...], gate[...], preferred_element_type=F32)
    u = jnp.dot(rows[...], up[...], preferred_element_type=F32)
    hidden = (jax.nn.silu(g) * u).astype(BF16)
    copies = []
    for n, at in enumerate(range(0, half, piece)):
        left = jnp.dot(hidden, down[:, at : at + piece], preferred_element_type=F32)
        right = jnp.dot(hidden, down[:, half + at : half + at + piece], preferred_element_type=F32)
        left = left.reshape(quads, 8, piece)
        right = right.reshape(quads, 8, piece)
        first = jnp.where(low(piece), left, pltpu.roll(right, 4, 1))
        second = jnp.where(low(piece), pltpu.roll(left, 4, 1), right)
        done[n] = jnp.stack([first, second], axis=1).reshape(total, piece).astype(BF16)
        copies.append(pltpu.make_async_copy(done.at[n], out.at[:, at : at + piece], sems.at[n]))
        copies[-1].start()
    for copy in copies:
        copy.wait()


def shared_kernel(normed, stream, gate, up, down, out):
    rows = normed[...]
    g = jnp.dot(rows, gate[...], preferred_element_type=F32)
    u = jnp.dot(rows, up[...], preferred_element_type=F32)
    hidden = (jax.nn.silu(g) * u).astype(BF16)
    part = jnp.dot(hidden, down[...], preferred_element_type=F32)

    @pl.when(pl.program_id(0) == 0)
    def _():
        out[...] = stream[...].astype(F32) + part

    @pl.when(pl.program_id(0) > 0)
    def _():
        out[...] += part


def gather_kernel(returned, meta, base, out, ready, sems):
    rows, half = returned.shape
    tokens = base.shape[0]
    piece = 256
    columns = jnp.transpose(meta[...])
    r = lax.broadcasted_iota(jnp.int32, (tokens, rows), 1)
    slots = ((r // 8) * 4 + r % 4).astype(F32)
    weight = jnp.where(
        slots == columns[:, 0:1],
        columns[:, 2:3],
        jnp.where(slots == columns[:, 1:2], columns[:, 3:4], 0.0),
    )
    lower = (r // 4) % 2 == 0
    weights = jnp.concatenate(
        [jnp.where(lower, weight, 0.0), jnp.where(lower, 0.0, weight)], axis=0
    ).astype(BF16)
    copies = []
    for n, at in enumerate(range(0, half, piece)):
        routed = jnp.dot(weights, returned[:, at : at + piece], preferred_element_type=F32)
        for h in range(2):
            k = 2 * n + h
            here = slice(h * half + at, h * half + at + piece)
            ready[k] = (base[:, here] + routed[h * tokens : (h + 1) * tokens, :]).astype(BF16)
            copies.append(pltpu.make_async_copy(ready.at[k], out.at[:, here], sems.at[k]))
            copies[-1].start()
    for copy in copies:
        copy.wait()


def whole(shape):
    zeros = (0,) * len(shape)
    return pl.BlockSpec(shape, lambda *_: zeros)


def held(x):
    return pltpu.with_memory_space_constraint(x, pltpu.VMEM), pl.BlockSpec(memory_space=pltpu.VMEM)


def copied(x, spec=None):
    return pltpu.with_memory_space_constraint(x, pltpu.HBM), spec or whole(x.shape)


def kernel(body, name, args, outs, us, grid=1, scratch=(), room=16):
    here = pl.BlockSpec(memory_space=pltpu.VMEM)
    return pl.pallas_call(
        body,
        grid=(grid,),
        in_specs=[spec for _, spec in args],
        out_specs=[here if spec is None else spec for _, _, spec in outs],
        out_shape=[
            (pltpu.VMEM if spec is None else pltpu.HBM)(shape, dtype)
            for shape, dtype, spec in outs
        ],
        scratch_shapes=scratch,
        cost_estimate=pl.CostEstimate(flops=int(us * 1e9), bytes_accessed=1000, transcendentals=0),
        compiler_params=pltpu.CompilerParams(vmem_limit_bytes=room * 2**20),
        name=name,
    )(*[x for x, _ in args])


def per_device(
    conv_value,
    conv_gate,
    taps,
    doc_ids,
    gn_gain,
    gn_shift,
    conv_out,
    residual,
    norm_gain,
    routes,
    route_weight,
    expert_gate,
    expert_up,
    expert_down,
    shared_gate,
    shared_up,
    shared_down,
):
    positions, channels = conv_value.shape
    tokens, model_width = residual.shape
    experts = expert_gate.shape[0] * lax.axis_size("sp") * lax.axis_size("tp")
    half = model_width // 2
    ids = doc_ids.reshape(1, positions)
    gain = gn_gain.reshape(1, channels)
    shift = gn_shift.reshape(1, channels)

    last = positions // HALO - 1
    tail = pl.BlockSpec((HALO, channels), lambda i: (last, 0))
    (packed,) = kernel(
        pack_kernel,
        "pack",
        [copied(conv_value, tail), copied(conv_gate, tail), copied(ids)],
        [((HALO, channels), BF16, None)],
        us=1,
    )
    halo = from_behind(packed, "sp", 1)
    (act,) = kernel(
        conv_kernel,
        "conv",
        [held(conv_value), held(conv_gate), held(taps), held(ids), held(gain), held(shift)],
        [((positions, channels), BF16, None)],
        us=4,
        scratch=[
            pltpu.VMEM((positions + 8, 128), F32),
            pltpu.VMEM((8, positions, 128), F32),
            pltpu.VMEM((positions, 128), F32),
        ],
    )
    keep, send = kernel(
        rim_kernel,
        "rim",
        [
            held(act),
            held(conv_value),
            held(conv_gate),
            held(taps),
            held(ids),
            held(halo),
            held(gain),
            held(shift),
        ],
        [((tokens, channels), BF16, None), ((tokens, channels), BF16, None)],
        us=0.3,
        scratch=[pltpu.VMEM((2 * HALO + 8, 128), F32), pltpu.VMEM((8, 2 * HALO, 128), F32)],
    )
    got = lax.ppermute(send, "tp", [(0, 1), (1, 0)])
    rows = (tokens, model_width)
    outside = pl.BlockSpec(memory_space=pltpu.HBM)
    meta, pick, part = kernel(
        route_kernel,
        "route",
        [held(routes.T), held(route_weight.T), held(keep), held(conv_out), held(residual)],
        [((8, tokens), F32, None), ((8 * experts, 2 * tokens), BF16, None), (rows, F32, None)],
        us=0.3,
    )
    stream, normed, outgoing = kernel(
        spread_kernel,
        "spread",
        [
            held(got),
            held(conv_out),
            held(part),
            held(norm_gain.reshape(1, model_width)),
            held(pick),
        ],
        [(rows, BF16, outside), (rows, BF16, outside), ((8 * experts, half), BF16, None)],
        us=3,
        scratch=[pltpu.VMEM(rows, BF16), pltpu.VMEM(rows, BF16), pltpu.SemaphoreType.DMA((2,))],
    )

    exchange = functools.partial(
        lax.all_to_all, axis_name=("sp", "tp"), split_axis=0, concat_axis=0, tiled=True
    )
    arrived = exchange(outgoing.reshape(experts, 8, half)).reshape(8 * experts, half)
    piece = 128
    by_column = pl.BlockSpec((model_width, piece), lambda i: (0, i))
    (base,) = kernel(
        shared_kernel,
        "shared",
        [
            copied(normed),
            copied(stream),
            copied(shared_gate, by_column),
            copied(shared_up, by_column),
            copied(shared_down, pl.BlockSpec((piece, model_width), lambda i: (i, 0))),
        ],
        [(rows, F32, None)],
        us=8,
        grid=shared_gate.shape[1] // piece,
    )
    (result,) = kernel(
        expert_kernel,
        "expert",
        [held(arrived), held(expert_gate[0]), held(expert_up[0]), held(expert_down[0])],
        [((8 * experts, half), BF16, outside)],
        us=5,
        scratch=[
            pltpu.VMEM((4 * experts, model_width), BF16),
            pltpu.VMEM((half // 256, 8 * experts, 256), BF16),
            pltpu.SemaphoreType.DMA((half // 256,)),
        ],
    )
    returned = exchange(result.reshape(experts, 8, half)).reshape(8 * experts, half)
    (out,) = kernel(
        gather_kernel,
        "gather",
        [held(returned), held(meta), held(base)],
        [(rows, BF16, outside)],
        us=2,
        scratch=[
            pltpu.VMEM((model_width // 256, tokens, 256), BF16),
            pltpu.SemaphoreType.DMA((model_width // 256,)),
        ],
    )
    return out


def solution(mesh):
    return jax.shard_map(
        per_device,
        mesh=mesh,
        in_specs=(
            P("sp", "tp"),
            P("sp", "tp"),
            P(None, "tp"),
            P("sp"),
            P("tp"),
            P("tp"),
            P(),
            P(("sp", "tp"), None),
            P(),
            P(("sp", "tp"), None),
            P(("sp", "tp"), None),
            P(("sp", "tp"), None, None),
            P(("sp", "tp"), None, None),
            P(("sp", "tp"), None, None),
            P(),
            P(),
            P(),
        ),
        out_specs=P(("sp", "tp"), None),
        check_vma=False,
    )
```
